32 devices in a mesh: sp: 8 (over z, y), tp: 4 (over x, core).
Axes of the slice: x: 2, y: 2, z: 4, core: 2. Of those that a mesh axis runs over, the one named last changes fastest.
Arguments:
- inputs: bfloat16 [8, 6144, 2048], P(None, ('sp', 'tp')), may hold values from -6 to 6
- norm_gain: bfloat16 [2048], replicated, may hold values from 0.099609375 to 1.8984375
- key_weight: bfloat16 [2048, 512], replicated, may hold values from -0.125 to 0.125
- value_weight: bfloat16 [2048, 512], replicated, may hold values from -0.125 to 0.125
- query: bfloat16 [8, 1024], P('sp', 'tp'), may hold values from -15 to 15
- head_bias: bfloat16 [16], P('tp'), may hold values from -14 to -6
Outputs:
- key_cache: bfloat16 [8, 6144, 512], P('sp', None, 'tp')
- value_cache: bfloat16 [8, 6144, 512], P('sp', None, 'tp')
- first_read: bfloat16 [8, 1024], P('sp', 'tp')
The draws below stay inside these ranges and needn't reach their ends.
All inputs are finite; a program needn't handle non-finite values.
Results may differ from the reference program's by a relative error of at most 0.012.
Values may be sent and summed in bfloat16 or wider, within the bound.
A program may use at most 128 MiB of HBM per device.

```python
import math
import jax
import jax.numpy as jnp
from jax import lax

D = 2048
HEAD_DIMENSION = 64
H = 16
KVH = 8
SEQS = 8
LEN = 6144


def draw_head_bias(key, part):
    order = jax.random.permutation(jax.random.fold_in(key, 11), H)
    spread = jax.random.uniform(jax.random.fold_in(key, 12), (H,), jnp.float32)
    slow_count = H // 2
    slow_heads = order < slow_count
    lift = math.exp(3.125)
    slow_bias = jnp.log(0.5 * jnp.power(4.0, spread) / (lift * LEN))
    fast_bias = jnp.log(0.01 * jnp.power(10.0 / 3.0, spread) / lift)
    return jnp.where(slow_heads, slow_bias, fast_bias).astype(jnp.float32).astype(jnp.bfloat16)


def levels(rng, dims, cuts, smallest, largest):
    def one(position, shards_of):
        draws = jax.random.uniform(jax.random.fold_in(jax.random.fold_in(rng, 6), position), (shards_of,), jnp.float32, smallest / len(cuts), largest / len(cuts))
        return jnp.repeat(jnp.exp(draws), dims[position] // shards_of).reshape((-1,) + (1,) * (len(dims) - position - 1))

    gain = one(*cuts[0])
    for cut in cuts[1:]:
        gain = gain * one(*cut)
    return gain


def noise(own_key, shape, scale, most, shards=(), dtype=jnp.bfloat16):
    drawn = jax.random.normal(own_key, shape, jnp.float32) * scale
    if len(shards) > 0:
        drawn = levels(own_key, shape, shards, -0.22, 0.18) * drawn
    return jnp.clip(drawn, min=-most, max=most).astype(dtype)


def setup_inputs(seed: int = 0) -> dict:
    splits = jax.random.split(jax.random.key(seed), 7)
    return {
        "inputs": noise(splits[0], (SEQS, LEN, D), 1.0, 6.0, ((1, 32),)),
        "norm_gain": jnp.clip(1.0 + 0.18 * jax.random.normal(splits[1], (D,), jnp.float32), 0.099609375, 1.8984375).astype(jnp.bfloat16),
        "key_weight": noise(splits[2], (D, KVH * HEAD_DIMENSION), D ** -0.5, 0.125),
        "value_weight": noise(splits[3], (D, KVH * HEAD_DIMENSION), D ** -0.5, 0.125),
        "query": noise(splits[4], (SEQS, H * HEAD_DIMENSION), 2.5, 15.0, ((0, 8), (1, 4))),
        "head_bias": draw_head_bias(jax.random.fold_in(splits[6], 71), 0),
    }


EPSILON = 1e-06

def one_read(operands, head_bias):
    query_row, key_rows, value_rows = operands
    repeat = H // KVH
    query_tensor = query_row.astype(jnp.float32).reshape(KVH, repeat, HEAD_DIMENSION)
    key_tensor = key_rows.astype(jnp.float32).reshape(LEN, KVH, HEAD_DIMENSION)
    value_tensor = value_rows.astype(jnp.float32).reshape(LEN, KVH, HEAD_DIMENSION)
    score_logits = jnp.einsum('ebx,uex->ebu', query_tensor, key_tensor) * HEAD_DIMENSION ** (-0.5)
    score_logits = score_logits + head_bias.astype(jnp.float32).reshape(KVH, repeat, 1)
    log_keep = jax.nn.log_sigmoid(-score_logits)
    suffix_logs = lax.cumsum(log_keep, axis=2, reverse=True) - log_keep
    stick_weights = jnp.exp(jax.nn.log_sigmoid(score_logits) + suffix_logs).astype(jnp.bfloat16)
    attended_output = jnp.einsum('euq,qec->euc', stick_weights.astype(jnp.float32), value_tensor)
    return attended_output.reshape(H * HEAD_DIMENSION).astype(jnp.bfloat16)

def reference(inputs, norm_gain, key_weight, value_weight, query, head_bias):
    widened = inputs.astype(jnp.float32)
    normed = widened * lax.rsqrt(lax.optimization_barrier(jnp.mean(widened * widened, axis=-1, keepdims=True)) + EPSILON)
    normed = (normed * norm_gain.astype(jnp.float32)).astype(jnp.bfloat16)
    flat_rows = normed.reshape(-1, D)
    key_cache = jnp.dot(flat_rows, key_weight, preferred_element_type=jnp.float32).astype(jnp.bfloat16)
    value_cache = jnp.dot(flat_rows, value_weight, preferred_element_type=jnp.float32).astype(jnp.bfloat16)
    key_cache = key_cache.reshape(SEQS, LEN, KVH * HEAD_DIMENSION)
    value_cache = value_cache.reshape(SEQS, LEN, KVH * HEAD_DIMENSION)
    first_read = lax.map(lambda operands: one_read(operands, head_bias), (query, key_cache, value_cache))
    return (key_cache, value_cache, first_read)
```

```python
import functools

import jax
import jax.numpy as jnp
from jax import lax
from jax.experimental import pallas as pl
from jax.experimental.pallas import tpu as pltpu
from jax.sharding import PartitionSpec as P

HEAD_DIMENSION = 64
EPSILON = 1e-06
LANES = 128
SUBLANES = 8
MESH = pl.DeviceIdType.MESH


def exchange_kernel(
    n_sp, n_tp, x_hbm, gain_ref, wk_hbm, wv_hbm, land_ref,
    x_buf, w_buf, send_buf, x_sem, w_sem, send_sem, recv_sem,
):
    sp, tp = lax.axis_index("sp"), lax.axis_index("tp")
    me = sp * n_tp + tp
    count = n_sp * n_tp
    span, cols = send_buf.shape[3], send_buf.shape[4]
    half = n_sp // 2

    def sequence_at(i):
        phase = i // half
        block = (sp // half + 1 + phase) % 2
        return block * half + (sp + i + phase) % half

    def x_copy(i):
        return pltpu.make_async_copy(x_hbm.at[sequence_at(i)], x_buf.at[i], x_sem.at[i])

    def w_copy(which):
        source = (wk_hbm, wv_hbm)[which]
        return pltpu.make_async_copy(source, w_buf.at[which], w_sem.at[which])

    x_copy(0).start()
    w_copy(0).start()
    w_copy(1).start()

    barrier = pltpu.get_barrier_semaphore()

    @pl.loop(1, count)
    def _(j):
        other = (me + j) % count
        pl.semaphore_signal(
            barrier, inc=1, device_id=(other // n_tp, other % n_tp), device_id_type=MESH
        )

    @pl.loop(1, n_sp)
    def _(i):
        x_copy(i).start()

    w_copy(0).wait()
    w_copy(1).wait()
    pl.semaphore_wait(barrier, count - 1)

    def send(i, g):
        return pltpu.make_async_remote_copy(
            src_ref=send_buf.at[i, g],
            dst_ref=land_ref.at[:, pl.ds(pl.multiple_of(me * span, span), span), :],
            send_sem=send_sem.at[i, g],
            recv_sem=recv_sem.at[sp, tp],
            device_id=(sequence_at(i), g),
            device_id_type=MESH,
        )

    @pl.loop(0, n_sp)
    def _(i):
        x_copy(i).wait()
        wide = x_buf[i].astype(jnp.float32)
        scale = lax.rsqrt(jnp.mean(wide * wide, axis=-1, keepdims=True) + EPSILON)
        normed = (wide * scale * gain_ref[...].astype(jnp.float32)).astype(jnp.bfloat16)
        for which in range(2):
            rows = jnp.dot(normed, w_buf[which], preferred_element_type=jnp.float32)
            rows = rows.astype(jnp.bfloat16)
            for g in range(n_tp):
                send_buf[i, g, which] = rows[:, g * cols:(g + 1) * cols]
        own = sequence_at(i) == sp
        for j in range(1, n_tp):
            send(i, (tp + j) % n_tp).start()

        @pl.when(jnp.logical_not(own))
        def _():
            send(i, tp).start()

        @pl.when(own)
        def _():
            land_ref[:, pl.ds(pl.multiple_of(me * span, span), span), :] = send_buf[i, tp]

    @pl.loop(1, count)
    def _(j):
        other = (me + j) % count
        pltpu.make_async_remote_copy(
            src_ref=send_buf.at[0, 0],
            dst_ref=land_ref.at[:, pl.ds(pl.multiple_of(other * span, span), span), :],
            send_sem=send_sem.at[0, 0],
            recv_sem=recv_sem.at[other // n_tp, other % n_tp],
            device_id=(sp, tp),
            device_id_type=MESH,
        ).wait_recv()

    @pl.loop(0, n_sp)
    def _(i):
        for j in range(1, n_tp):
            send(i, (tp + j) % n_tp).wait_send()

        @pl.when(sequence_at(i) != sp)
        def _():
            send(i, tp).wait_send()


def read_kernel(repeat, land_ref, query_ref, bias_ref, key_out, value_out, read_ref, sem):
    copies = [
        pltpu.make_async_copy(land_ref.at[0], key_out.at[0], sem.at[0]),
        pltpu.make_async_copy(land_ref.at[1], value_out.at[0], sem.at[1]),
    ]
    for copy in copies:
        copy.start()
    rows = query_ref.shape[0]
    length = land_ref.shape[1]
    chunks = length // LANES
    score = lax.dot_general(
        query_ref[...], land_ref[0], (((1,), (1,)), ((), ())),
        preferred_element_type=jnp.float32,
    )
    score = score + bias_ref[:, 0:1]
    keep = -(jnp.maximum(score, 0.0) + jnp.log1p(jnp.exp(-jnp.abs(score))))
    stacked = jnp.concatenate(
        [keep[:, c * LANES:(c + 1) * LANES] for c in range(chunks)], axis=0
    )
    source = lax.broadcasted_iota(jnp.int32, (LANES, LANES), 0)
    target = lax.broadcasted_iota(jnp.int32, (LANES, LANES), 1)
    later = (source > target).astype(jnp.float32)
    inside = jnp.dot(stacked, later, precision=lax.Precision.HIGHEST)
    total = jnp.dot(stacked, jnp.ones_like(later), precision=lax.Precision.HIGHEST)
    carry = jnp.zeros((rows, LANES), jnp.float32)
    pieces = [None] * chunks
    for c in reversed(range(chunks)):
        pieces[c] = inside[c * rows:(c + 1) * rows] + carry
        carry = carry + total[c * rows:(c + 1) * rows]
    weight = jnp.exp(score + keep + jnp.concatenate(pieces, axis=1)).astype(jnp.bfloat16)
    read = jnp.dot(weight, land_ref[1], preferred_element_type=jnp.float32)
    heads = read_ref.shape[1] // HEAD_DIMENSION
    parts = []
    for h in range(heads):
        left = (h // repeat) * HEAD_DIMENSION
        parts.append(read[h:h + 1, left:left + HEAD_DIMENSION])
    read_ref[...] = jnp.concatenate(parts, axis=1).astype(jnp.bfloat16)
    for copy in copies:
        copy.wait()


def body(n_sp, n_tp, inputs, norm_gain, key_weight, value_weight, query, head_bias):
    seqs, span, width = inputs.shape
    cols = key_weight.shape[1] // n_tp
    kv_heads = cols // HEAD_DIMENSION
    q_heads = query.shape[1] // HEAD_DIMENSION
    repeat = q_heads // kv_heads
    length = span * n_sp * n_tp
    hbm = pl.BlockSpec(memory_space=pl.ANY)
    vmem = pl.BlockSpec(memory_space=pltpu.VMEM)
    landed = pl.pallas_call(
        functools.partial(exchange_kernel, n_sp, n_tp),
        out_shape=jax.ShapeDtypeStruct((2, length, cols), jnp.bfloat16),
        in_specs=[hbm, vmem, hbm, hbm],
        out_specs=vmem,
        scratch_shapes=[
            pltpu.VMEM((seqs, span, width), jnp.bfloat16),
            pltpu.VMEM((2, width, key_weight.shape[1]), jnp.bfloat16),
            pltpu.VMEM((n_sp, n_tp, 2, span, cols), jnp.bfloat16),
            pltpu.SemaphoreType.DMA((n_sp,)),
            pltpu.SemaphoreType.DMA((2,)),
            pltpu.SemaphoreType.DMA((n_sp, n_tp)),
            pltpu.SemaphoreType.DMA((n_sp, n_tp)),
        ],
        compiler_params=pltpu.CompilerParams(
            collective_id=0, has_side_effects=True, vmem_limit_bytes=56 * 2**20
        ),
    )(inputs, norm_gain.reshape(1, width), key_weight, value_weight)

    pad = -q_heads % SUBLANES
    scaled = query.reshape(q_heads, HEAD_DIMENSION) * jnp.bfloat16(HEAD_DIMENSION ** -0.5)
    owner = (jnp.arange(q_heads) // repeat)[:, None] == jnp.arange(kv_heads)[None, :]
    spread = jnp.where(owner[:, :, None], scaled[:, None, :], jnp.bfloat16(0))
    spread = jnp.pad(spread.reshape(q_heads, cols), ((0, pad), (0, 0)))
    bias = jnp.pad(head_bias.astype(jnp.float32), (0, pad))
    bias = jnp.broadcast_to(bias[:, None], (q_heads + pad, LANES))
    return pl.pallas_call(
        functools.partial(read_kernel, repeat),
        out_shape=(
            jax.ShapeDtypeStruct((1, length, cols), jnp.bfloat16),
            jax.ShapeDtypeStruct((1, length, cols), jnp.bfloat16),
            jax.ShapeDtypeStruct((1, q_heads * HEAD_DIMENSION), jnp.bfloat16),
        ),
        in_specs=[vmem, vmem, vmem],
        out_specs=(hbm, hbm, vmem),
        scratch_shapes=[pltpu.SemaphoreType.DMA((2,))],
    )(landed, spread, bias)


def solution(mesh):
    placed = (P(None, ("sp", "tp"), None), P(), P(), P(), P("sp", "tp"), P("tp"))
    return jax.shard_map(
        functools.partial(body, mesh.shape["sp"], mesh.shape["tp"]),
        mesh=mesh,
        in_specs=placed,
        out_specs=(P("sp", None, "tp"), P("sp", None, "tp"), P("sp", "tp")),
        check_vma=False,
    )
```

```python
import functools

import jax
import jax.numpy as jnp
from jax import lax
from jax.experimental import pallas as pl
from jax.experimental.pallas import tpu as pltpu
from jax.sharding import PartitionSpec as P

HEAD_DIMENSION = 64
EPSILON = 1e-06
LANES = 128
SUBLANES = 8
WRITES = 4
VMEM_BYTES = 67043328
MESH = pl.DeviceIdType.MESH


def group_at(n_sp, sp, i):
    half = n_sp // 2
    block = (sp // half + i // half) % 2
    return block * half + (sp + half - i % half) % half


def spread_query(query_ref, heads, repeat, cols):
    scaled = query_ref[...].astype(jnp.float32) * HEAD_DIMENSION ** -0.5
    rows = []
    for h in range(heads):
        pieces = [jnp.zeros((1, HEAD_DIMENSION), jnp.float32)] * (cols // HEAD_DIMENSION)
        pieces[h // repeat] = scaled[:, h * HEAD_DIMENSION:(h + 1) * HEAD_DIMENSION]
        rows.append(jnp.concatenate(pieces, axis=1))
    rows.append(jnp.zeros((-heads % SUBLANES, cols), jnp.float32))
    return jnp.concatenate(rows, axis=0).astype(jnp.bfloat16)


def bias_column(bias_ref, rows):
    heads = bias_ref.shape[0]
    wide = jnp.broadcast_to(bias_ref[...].astype(jnp.float32).reshape(1, heads), (rows, heads))
    row = lax.broadcasted_iota(jnp.int32, (rows, heads), 0)
    col = lax.broadcasted_iota(jnp.int32, (rows, heads), 1)
    return jnp.sum(jnp.where(row == col, wide, 0.0), axis=1, keepdims=True)


def group_read(spread, bias, keys, values):
    rows = spread.shape[0]
    chunks = keys.shape[0] // LANES
    score = lax.dot_general(
        spread, keys, (((1,), (1,)), ((), ())), preferred_element_type=jnp.float32
    )
    score = score + bias
    keep = -(jnp.maximum(score, 0.0) + jnp.log1p(jnp.exp(-jnp.abs(score))))
    stacked = jnp.concatenate(
        [keep[:, c * LANES:(c + 1) * LANES] for c in range(chunks)], axis=0
    )
    source = lax.broadcasted_iota(jnp.int32, (LANES, LANES), 0)
    target = lax.broadcasted_iota(jnp.int32, (LANES, LANES), 1)
    later = (source > target).astype(jnp.float32)
    inside = jnp.dot(stacked, later, precision=lax.Precision.HIGHEST)
    total = jnp.dot(stacked, jnp.ones_like(later), precision=lax.Precision.HIGHEST)
    carry = jnp.zeros((rows, LANES), jnp.float32)
    pieces = [None] * chunks
    for c in reversed(range(chunks)):
        pieces[c] = inside[c * rows:(c + 1) * rows] + carry
        carry = carry + total[c * rows:(c + 1) * rows]
    weight = jnp.exp(score + keep + jnp.concatenate(pieces, axis=1)).astype(jnp.bfloat16)
    read = jnp.dot(weight, values, preferred_element_type=jnp.float32)
    return read, jnp.broadcast_to(carry[:, 0:1], read.shape)


def exchange_kernel(
    n_sp, n_tp, repeat, x_hbm, gain_hbm, wk_hbm, wv_hbm, query_hbm, bias_hbm,
    land_ref, part_ref, x_buf, w_buf, gain_ref, query_ref, bias_ref, send_buf,
    x_sem, w_sem, small_sem, send_sem, recv_sem,
):
    sp, tp = lax.axis_index("sp"), lax.axis_index("tp")
    me = sp * n_tp + tp
    count = n_sp * n_tp
    span, cols = send_buf.shape[3], send_buf.shape[4]
    half = n_sp // 2
    triples = half // 2

    def sequence_at(i):
        late = i // (3 * triples)
        triple, place = i // 3, i % 3
        near = late + (1 - late) * (place // 2)
        far_offset = 2 * triple + place
        near_offset = triples + late * (i - half) + (1 - late) * triple
        offset = near * near_offset + (1 - near) * far_offset
        return ((sp // half + 1 + near) % 2) * half + (sp + offset) % half

    def x_copy(i):
        return pltpu.make_async_copy(x_hbm.at[sequence_at(i)], x_buf.at[i], x_sem.at[i])

    def w_copy(which):
        source = (wk_hbm, wv_hbm)[which]
        return pltpu.make_async_copy(source, w_buf.at[which], w_sem.at[which])

    small = [
        pltpu.make_async_copy(source, buffer, small_sem.at[k])
        for k, (source, buffer) in enumerate(
            ((gain_hbm, gain_ref), (query_hbm, query_ref), (bias_hbm, bias_ref))
        )
    ]
    barrier = pltpu.get_barrier_semaphore()

    @pl.loop(1, count)
    def _(j):
        other = (me + j) % count
        pl.semaphore_signal(
            barrier, inc=1, device_id=(other // n_tp, other % n_tp), device_id_type=MESH
        )

    small[0].start()
    x_copy(0).start()
    w_copy(0).start()
    w_copy(1).start()
    small[1].start()
    small[2].start()

    @pl.loop(1, n_sp)
    def _(i):
        x_copy(i).start()

    for copy in small:
        copy.wait()
    gain = gain_ref[...].astype(jnp.float32).reshape(1, gain_ref.shape[0])

    def compute(i, first):
        x_copy(i).wait()
        wide = x_buf[i].astype(jnp.float32)
        scale = lax.rsqrt(jnp.mean(wide * wide, axis=-1, keepdims=True) + EPSILON)
        normed = (wide * scale * gain).astype(jnp.bfloat16)
        for which in range(2):
            if first:
                w_copy(which).wait()
            rows = jnp.dot(normed, w_buf[which], preferred_element_type=jnp.float32)
            rows = rows.astype(jnp.bfloat16)
            for g in range(n_tp):
                send_buf[i, g, which] = rows[:, g * cols:(g + 1) * cols]

    def own_rows(source):
        return pl.ds(pl.multiple_of(source * span, span), span)

    def send(i, g):
        return pltpu.make_async_remote_copy(
            src_ref=send_buf.at[i, g],
            dst_ref=land_ref.at[:, own_rows(me), :],
            send_sem=send_sem.at[i, g],
            recv_sem=recv_sem.at[sp, tp],
            device_id=(sequence_at(i), g),
            device_id_type=MESH,
        )

    def send_all(i):
        own = sequence_at(i) == sp
        for j in range(1, n_tp):
            send(i, (tp + j) % n_tp).start()

        @pl.when(jnp.logical_not(own))
        def _():
            send(i, tp).start()

        @pl.when(own)
        def _():
            land_ref[:, own_rows(me), :] = send_buf[i, tp]

    compute(0, True)
    pl.semaphore_wait(barrier, count - 1)
    send_all(0)

    @pl.loop(1, n_sp)
    def _(i):
        compute(i, False)
        send_all(i)

    heads = query_ref.shape[1] // HEAD_DIMENSION
    spread = spread_query(query_ref, heads, repeat, cols)
    bias = bias_column(bias_ref, spread.shape[0])
    group_rows = n_tp * span

    def arrive(source):
        for g in range(n_tp):
            @pl.when(source * n_tp + g != me)
            def _():
                pltpu.make_async_remote_copy(
                    src_ref=send_buf.at[0, 0],
                    dst_ref=land_ref.at[:, own_rows(source * n_tp + g), :],
                    send_sem=send_sem.at[0, 0],
                    recv_sem=recv_sem.at[source, g],
                    device_id=(source, g),
                    device_id_type=MESH,
                ).wait_recv()

    @pl.loop(0, n_sp - 1)
    def _(i):
        source = group_at(n_sp, sp, i)
        arrive(source)
        at = pl.ds(pl.multiple_of(source * group_rows, group_rows), group_rows)
        read, total = group_read(spread, bias, land_ref[0, at, :], land_ref[1, at, :])
        part_ref[source, 0] = read
        part_ref[source, 1] = total

    part_ref[n_sp, 0] = spread.astype(jnp.float32)
    part_ref[n_sp, 1] = jnp.broadcast_to(bias, spread.shape)
    last = group_at(n_sp, sp, n_sp - 1)
    part_ref[last] = jnp.zeros(part_ref.shape[1:], jnp.float32)

    @pl.loop(0, n_sp)
    def _(i):
        for j in range(1, n_tp):
            send(i, (tp + j) % n_tp).wait_send()

        @pl.when(sequence_at(i) != sp)
        def _():
            send(i, tp).wait_send()

    arrive(last)


def write_kernel(
    n_sp, repeat, land_ref, part_ref, key_out, value_out, read_ref, part, sem
):
    length, cols = land_ref.shape[1:]
    copies = []
    for which, out in enumerate((key_out, value_out)):
        for c in range(WRITES):
            at = pl.ds(c * (length // WRITES), length // WRITES)
            copies.append(
                pltpu.make_async_copy(land_ref.at[which, at], out.at[0, at], sem.at[which, c])
            )
    for copy in copies:
        copy.start()
    heads = read_ref.shape[1] // HEAD_DIMENSION
    group_rows = length // n_sp
    spread = part_ref[n_sp, 0].astype(jnp.bfloat16)
    bias = part_ref[n_sp, 1][:, 0:1]
    last = group_at(n_sp, lax.axis_index("sp"), n_sp - 1)
    at = pl.ds(pl.multiple_of(last * group_rows, group_rows), group_rows)
    read, total = group_read(spread, bias, land_ref[0, at, :], land_ref[1, at, :])
    part[...] = part_ref[0:n_sp]
    part[last, 0] = read
    part[last, 1] = total
    after = jnp.zeros_like(total)
    whole = jnp.zeros_like(read)
    for p in reversed(range(n_sp)):
        whole = whole + jnp.exp(after) * part[p, 0]
        after = after + part[p, 1]
    pieces = []
    for h in range(heads):
        left = (h // repeat) * HEAD_DIMENSION
        pieces.append(whole[h:h + 1, left:left + HEAD_DIMENSION])
    read_ref[...] = jnp.concatenate(pieces, axis=1).astype(jnp.bfloat16)
    for copy in copies:
        copy.wait()


def body(n_sp, n_tp, inputs, norm_gain, key_weight, value_weight, query, head_bias):
    seqs, span, width = inputs.shape
    cols = key_weight.shape[1] // n_tp
    q_heads = query.shape[1] // HEAD_DIMENSION
    repeat = q_heads // (cols // HEAD_DIMENSION)
    length = span * n_sp * n_tp
    rows = q_heads + -q_heads % SUBLANES
    lanes = cols + -cols % LANES
    kept = 2 * length * lanes * 2 + (n_sp + 1) * 2 * rows * lanes * 4
    hbm = pl.BlockSpec(memory_space=pltpu.HBM)
    vmem = pl.BlockSpec(memory_space=pltpu.VMEM)
    landed, parts = pl.pallas_call(
        functools.partial(exchange_kernel, n_sp, n_tp, repeat),
        out_shape=(
            pltpu.VMEM((2, length, cols), jnp.bfloat16),
            pltpu.VMEM((n_sp + 1, 2, rows, cols), jnp.float32),
        ),
        in_specs=[hbm] * 6,
        out_specs=(vmem, vmem),
        scratch_shapes=[
            pltpu.VMEM((seqs, span, width), jnp.bfloat16),
            pltpu.VMEM((2, width, key_weight.shape[1]), jnp.bfloat16),
            pltpu.VMEM(norm_gain.shape, norm_gain.dtype),
            pltpu.VMEM(query.shape, query.dtype),
            pltpu.VMEM(head_bias.shape, head_bias.dtype),
            pltpu.VMEM((n_sp, n_tp, 2, span, cols), jnp.bfloat16),
            pltpu.SemaphoreType.DMA((n_sp,)),
            pltpu.SemaphoreType.DMA((2,)),
            pltpu.SemaphoreType.DMA((3,)),
            pltpu.SemaphoreType.DMA((n_sp, n_tp)),
            pltpu.SemaphoreType.DMA((n_sp, n_tp)),
        ],
        compiler_params=pltpu.CompilerParams(
            collective_id=0, has_side_effects=True, vmem_limit_bytes=VMEM_BYTES - kept
        ),
    )(inputs, norm_gain, key_weight, value_weight, query, head_bias)
    return pl.pallas_call(
        functools.partial(write_kernel, n_sp, repeat),
        out_shape=(
            jax.ShapeDtypeStruct((1, length, cols), jnp.bfloat16),
            jax.ShapeDtypeStruct((1, length, cols), jnp.bfloat16),
            jax.ShapeDtypeStruct((1, q_heads * HEAD_DIMENSION), jnp.bfloat16),
        ),
        in_specs=[vmem, vmem],
        out_specs=(hbm, hbm, vmem),
        scratch_shapes=[
            pltpu.VMEM((n_sp, 2, rows, cols), jnp.float32),
            pltpu.SemaphoreType.DMA((2, WRITES)),
        ],
        compiler_params=pltpu.CompilerParams(vmem_limit_bytes=16 * 2**20),
    )(landed, parts)


def solution(mesh):
    placed = (P(None, ("sp", "tp"), None), P(), P(), P(), P("sp", "tp"), P("tp"))
    return jax.shard_map(
        functools.partial(body, mesh.shape["sp"], mesh.shape["tp"]),
        mesh=mesh,
        in_specs=placed,
        out_specs=(P("sp", None, "tp"), P("sp", None, "tp"), P("sp", "tp")),
        check_vma=False,
    )
```

```python
import functools

import jax
import jax.numpy as jnp
from jax import lax
from jax.experimental import pallas as pl
from jax.experimental.pallas import tpu as pltpu
from jax.sharding import PartitionSpec as P

HEAD_DIMENSION = 64
EPSILON = 1e-06
LANES = 128
SUBLANES = 8
WRITES = 4
VMEM_BYTES = 67043328
MESH = pl.DeviceIdType.MESH


def flip(index, mask, size):
    bits = [1 << b for b in range((size - 1).bit_length())]
    return sum(((index // bit + mask // bit) % 2) * bit for bit in bits)


def far_mask(half, a):
    return half + (a % 2) * (half // 2) + a // 2


def send_mask(n_sp, i):
    half = n_sp // 2
    quarter = half // 2
    late = i // (3 * quarter)
    triple, place = i // 3, i % 3
    near = late + (1 - late) * (place // 2)
    q = late * (i - half) + (1 - late) * triple
    second = q // quarter
    near_mask = (1 - second) * (quarter + q) + second * (half - 1 - q)
    return near * near_mask + (1 - near) * far_mask(half, 2 * triple + place)


def read_mask(n_sp, i):
    half = n_sp // 2
    late = i // half
    return (1 - late) * i + late * far_mask(half, i - half)


def spread_query(query_ref, heads, repeat, cols):
    scaled = query_ref[...].astype(jnp.float32) * HEAD_DIMENSION ** -0.5
    rows = []
    for h in range(heads):
        pieces = [jnp.zeros((1, HEAD_DIMENSION), jnp.float32)] * (cols // HEAD_DIMENSION)
        pieces[h // repeat] = scaled[:, h * HEAD_DIMENSION:(h + 1) * HEAD_DIMENSION]
        rows.append(jnp.concatenate(pieces, axis=1))
    rows.append(jnp.zeros((-heads % SUBLANES, cols), jnp.float32))
    return jnp.concatenate(rows, axis=0).astype(jnp.bfloat16)


def bias_column(bias_ref, rows):
    heads = bias_ref.shape[0]
    wide = jnp.broadcast_to(bias_ref[...].astype(jnp.float32).reshape(1, heads), (rows, heads))
    row = lax.broadcasted_iota(jnp.int32, (rows, heads), 0)
    col = lax.broadcasted_iota(jnp.int32, (rows, heads), 1)
    return jnp.sum(jnp.where(row == col, wide, 0.0), axis=1, keepdims=True)


def group_read(spread, bias, keys, values):
    rows = spread.shape[0]
    chunks = keys.shape[0] // LANES
    score = lax.dot_general(
        spread, keys, (((1,), (1,)), ((), ())), preferred_element_type=jnp.float32
    )
    score = score + bias
    keep = -(jnp.maximum(score, 0.0) + jnp.log1p(jnp.exp(-jnp.abs(score))))
    stacked = jnp.concatenate(
        [keep[:, c * LANES:(c + 1) * LANES] for c in range(chunks)], axis=0
    )
    source = lax.broadcasted_iota(jnp.int32, (LANES, LANES), 0)
    target = lax.broadcasted_iota(jnp.int32, (LANES, LANES), 1)
    later = (source > target).astype(jnp.float32)
    inside = jnp.dot(stacked, later, precision=lax.Precision.HIGHEST)
    total = jnp.dot(stacked, jnp.ones_like(later), precision=lax.Precision.HIGHEST)
    carry = jnp.zeros((rows, LANES), jnp.float32)
    pieces = [None] * chunks
    for c in reversed(range(chunks)):
        pieces[c] = inside[c * rows:(c + 1) * rows] + carry
        carry = carry + total[c * rows:(c + 1) * rows]
    weight = jnp.exp(score + keep + jnp.concatenate(pieces, axis=1)).astype(jnp.bfloat16)
    read = jnp.dot(weight, values, preferred_element_type=jnp.float32)
    return read, jnp.broadcast_to(carry[:, 0:1], read.shape)


def exchange_kernel(
    n_sp, n_tp, repeat, x_hbm, gain_hbm, wk_hbm, wv_hbm, query_hbm, bias_hbm,
    land_ref, part_ref, x_buf, w_buf, gain_ref, query_ref, bias_ref, send_buf,
    x_sem, w_sem, small_sem, send_sem, recv_sem,
):
    sp, tp = lax.axis_index("sp"), lax.axis_index("tp")
    me = sp * n_tp + tp
    count = n_sp * n_tp
    span, cols = send_buf.shape[3], send_buf.shape[4]

    def sequence_at(i):
        return flip(sp, send_mask(n_sp, i), n_sp)

    def x_copy(i):
        return pltpu.make_async_copy(x_hbm.at[sequence_at(i)], x_buf.at[i], x_sem.at[i])

    def w_copy(which):
        source = (wk_hbm, wv_hbm)[which]
        return pltpu.make_async_copy(source, w_buf.at[which], w_sem.at[which])

    small = [
        pltpu.make_async_copy(source, buffer, small_sem.at[k])
        for k, (source, buffer) in enumerate(
            ((gain_hbm, gain_ref), (query_hbm, query_ref), (bias_hbm, bias_ref))
        )
    ]
    barrier = pltpu.get_barrier_semaphore()

    @pl.loop(1, count)
    def _(j):
        other = (me + j) % count
        pl.semaphore_signal(
            barrier, inc=1, device_id=(other // n_tp, other % n_tp), device_id_type=MESH
        )

    small[0].start()
    x_copy(0).start()
    w_copy(0).start()
    w_copy(1).start()
    small[1].start()
    small[2].start()

    @pl.loop(1, n_sp)
    def _(i):
        x_copy(i).start()

    for copy in small:
        copy.wait()
    gain = gain_ref[...].astype(jnp.float32).reshape(1, gain_ref.shape[0])

    def compute(i, first):
        x_copy(i).wait()
        wide = x_buf[i].astype(jnp.float32)
        scale = lax.rsqrt(jnp.mean(wide * wide, axis=-1, keepdims=True) + EPSILON)
        normed = (wide * scale * gain).astype(jnp.bfloat16)
        for which in range(2):
            if first:
                w_copy(which).wait()
            rows = jnp.dot(normed, w_buf[which], preferred_element_type=jnp.float32)
            rows = rows.astype(jnp.bfloat16)
            for g in range(n_tp):
                send_buf[i, g, which] = rows[:, g * cols:(g + 1) * cols]

    def own_rows(source):
        return pl.ds(pl.multiple_of(source * span, span), span)

    def send(i, g):
        return pltpu.make_async_remote_copy(
            src_ref=send_buf.at[i, g],
            dst_ref=land_ref.at[:, own_rows(me), :],
            send_sem=send_sem.at[i, g],
            recv_sem=recv_sem.at[sp, tp],
            device_id=(sequence_at(i), g),
            device_id_type=MESH,
        )

    def send_all(i):
        own = sequence_at(i) == sp
        for j in range(1, n_tp):
            send(i, flip(tp, j, n_tp)).start()

        @pl.when(jnp.logical_not(own))
        def _():
            send(i, tp).start()

        @pl.when(own)
        def _():
            land_ref[:, own_rows(me), :] = send_buf[i, tp]

    compute(0, True)
    pl.semaphore_wait(barrier, count - 1)
    send_all(0)

    @pl.loop(1, n_sp)
    def _(i):
        compute(i, False)
        send_all(i)

    heads = query_ref.shape[1] // HEAD_DIMENSION
    spread = spread_query(query_ref, heads, repeat, cols)
    bias = bias_column(bias_ref, spread.shape[0])
    group_rows = n_tp * span

    def arrive(source):
        for g in range(n_tp):
            @pl.when(source * n_tp + g != me)
            def _():
                pltpu.make_async_remote_copy(
                    src_ref=send_buf.at[0, 0],
                    dst_ref=land_ref.at[:, own_rows(source * n_tp + g), :],
                    send_sem=send_sem.at[0, 0],
                    recv_sem=recv_sem.at[source, g],
                    device_id=(source, g),
                    device_id_type=MESH,
                ).wait_recv()

    @pl.loop(0, n_sp - 1)
    def _(i):
        source = flip(sp, read_mask(n_sp, i), n_sp)
        arrive(source)
        at = pl.ds(pl.multiple_of(source * group_rows, group_rows), group_rows)
        read, total = group_read(spread, bias, land_ref[0, at, :], land_ref[1, at, :])
        part_ref[source, 0] = read
        part_ref[source, 1] = total

    part_ref[n_sp, 0] = spread.astype(jnp.float32)
    part_ref[n_sp, 1] = jnp.broadcast_to(bias, spread.shape)
    last = flip(sp, n_sp - 1, n_sp)
    part_ref[last] = jnp.zeros(part_ref.shape[1:], jnp.float32)

    @pl.loop(0, n_sp)
    def _(i):
        for j in range(1, n_tp):
            send(i, flip(tp, j, n_tp)).wait_send()

        @pl.when(sequence_at(i) != sp)
        def _():
            send(i, tp).wait_send()

    arrive(last)


def write_kernel(
    n_sp, repeat, land_ref, part_ref, key_out, value_out, read_ref, part, sem
):
    length, cols = land_ref.shape[1:]
    copies = []
    for which, out in enumerate((key_out, value_out)):
        for c in range(WRITES):
            at = pl.ds(c * (length // WRITES), length // WRITES)
            copies.append(
                pltpu.make_async_copy(land_ref.at[which, at], out.at[0, at], sem.at[which, c])
            )
    for copy in copies:
        copy.start()
    heads = read_ref.shape[1] // HEAD_DIMENSION
    group_rows = length // n_sp
    spread = part_ref[n_sp, 0].astype(jnp.bfloat16)
    bias = part_ref[n_sp, 1][:, 0:1]
    last = flip(lax.axis_index("sp"), n_sp - 1, n_sp)
    at = pl.ds(pl.multiple_of(last * group_rows, group_rows), group_rows)
    read, total = group_read(spread, bias, land_ref[0, at, :], land_ref[1, at, :])
    part[...] = part_ref[0:n_sp]
    part[last, 0] = read
    part[last, 1] = total
    after = jnp.zeros_like(total)
    whole = jnp.zeros_like(read)
    for p in reversed(range(n_sp)):
        whole = whole + jnp.exp(after) * part[p, 0]
        after = after + part[p, 1]
    pieces = []
    for h in range(heads):
        left = (h // repeat) * HEAD_DIMENSION
        pieces.append(whole[h:h + 1, left:left + HEAD_DIMENSION])
    read_ref[...] = jnp.concatenate(pieces, axis=1).astype(jnp.bfloat16)
    for copy in copies:
        copy.wait()


def body(n_sp, n_tp, inputs, norm_gain, key_weight, value_weight, query, head_bias):
    seqs, span, width = inputs.shape
    cols = key_weight.shape[1] // n_tp
    q_heads = query.shape[1] // HEAD_DIMENSION
    repeat = q_heads // (cols // HEAD_DIMENSION)
    length = span * n_sp * n_tp
    rows = q_heads + -q_heads % SUBLANES
    lanes = cols + -cols % LANES
    kept = 2 * length * lanes * 2 + (n_sp + 1) * 2 * rows * lanes * 4
    hbm = pl.BlockSpec(memory_space=pltpu.HBM)
    vmem = pl.BlockSpec(memory_space=pltpu.VMEM)
    landed, parts = pl.pallas_call(
        functools.partial(exchange_kernel, n_sp, n_tp, repeat),
        out_shape=(
            pltpu.VMEM((2, length, cols), jnp.bfloat16),
            pltpu.VMEM((n_sp + 1, 2, rows, cols), jnp.float32),
        ),
        in_specs=[hbm] * 6,
        out_specs=(vmem, vmem),
        scratch_shapes=[
            pltpu.VMEM((seqs, span, width), jnp.bfloat16),
            pltpu.VMEM((2, width, key_weight.shape[1]), jnp.bfloat16),
            pltpu.VMEM(norm_gain.shape, norm_gain.dtype),
            pltpu.VMEM(query.shape, query.dtype),
            pltpu.VMEM(head_bias.shape, head_bias.dtype),
            pltpu.VMEM((n_sp, n_tp, 2, span, cols), jnp.bfloat16),
            pltpu.SemaphoreType.DMA((n_sp,)),
            pltpu.SemaphoreType.DMA((2,)),
            pltpu.SemaphoreType.DMA((3,)),
            pltpu.SemaphoreType.DMA((n_sp, n_tp)),
            pltpu.SemaphoreType.DMA((n_sp, n_tp)),
        ],
        compiler_params=pltpu.CompilerParams(
            collective_id=0, has_side_effects=True, vmem_limit_bytes=VMEM_BYTES - kept
        ),
    )(inputs, norm_gain, key_weight, value_weight, query, head_bias)
    return pl.pallas_call(
        functools.partial(write_kernel, n_sp, repeat),
        out_shape=(
            jax.ShapeDtypeStruct((1, length, cols), jnp.bfloat16),
            jax.ShapeDtypeStruct((1, length, cols), jnp.bfloat16),
            jax.ShapeDtypeStruct((1, q_heads * HEAD_DIMENSION), jnp.bfloat16),
        ),
        in_specs=[vmem, vmem],
        out_specs=(hbm, hbm, vmem),
        scratch_shapes=[
            pltpu.VMEM((n_sp, 2, rows, cols), jnp.float32),
            pltpu.SemaphoreType.DMA((2, WRITES)),
        ],
        compiler_params=pltpu.CompilerParams(vmem_limit_bytes=16 * 2**20),
    )(landed, parts)


def solution(mesh):
    placed = (P(None, ("sp", "tp"), None), P(), P(), P(), P("sp", "tp"), P("tp"))
    return jax.shard_map(
        functools.partial(body, mesh.shape["sp"], mesh.shape["tp"]),
        mesh=mesh,
        in_specs=placed,
        out_specs=(P("sp", None, "tp"), P("sp", None, "tp"), P("sp", "tp")),
        check_vma=False,
    )
```

```python
import functools

import jax
import jax.numpy as jnp
from jax import lax
from jax.experimental import pallas as pl
from jax.experimental.pallas import tpu as pltpu
from jax.sharding import PartitionSpec as P

HEAD_DIMENSION = 64
EPSILON = 1e-06
LANES = 128
SUBLANES = 8
WRITES = 4
VMEM_BYTES = 67043328
MESH = pl.DeviceIdType.MESH


def flip(index, mask, size):
    bits = [1 << b for b in range((size - 1).bit_length())]
    return sum(((index // bit + mask // bit) % 2) * bit for bit in bits)


def far_mask(half, a):
    return half + (a % 2) * (half // 2) + a // 2


def send_mask(n_sp, i):
    half = n_sp // 2
    quarter = half // 2
    late = i // (3 * quarter)
    triple, place = i // 3, i % 3
    near = late + (1 - late) * (place // 2)
    q = late * (i - half) + (1 - late) * triple
    second = q // quarter
    near_mask = (1 - second) * (quarter + q) + second * (half - 1 - q)
    return near * near_mask + (1 - near) * far_mask(half, 2 * triple + place)


def read_mask(n_sp, i):
    half = n_sp // 2
    late = i // half
    return (1 - late) * i + late * far_mask(half, i - half)


def spread_query(query_ref, heads, repeat, cols):
    scaled = query_ref[...].astype(jnp.float32) * HEAD_DIMENSION ** -0.5
    rows = []
    for h in range(heads):
        pieces = [jnp.zeros((1, HEAD_DIMENSION), jnp.float32)] * (cols // HEAD_DIMENSION)
        pieces[h // repeat] = scaled[:, h * HEAD_DIMENSION:(h + 1) * HEAD_DIMENSION]
        rows.append(jnp.concatenate(pieces, axis=1))
    rows.append(jnp.zeros((-heads % SUBLANES, cols), jnp.float32))
    return jnp.concatenate(rows, axis=0).astype(jnp.bfloat16)


def bias_column(bias_ref, rows):
    heads = bias_ref.shape[0]
    wide = jnp.broadcast_to(bias_ref[...].astype(jnp.float32).reshape(1, heads), (rows, heads))
    row = lax.broadcasted_iota(jnp.int32, (rows, heads), 0)
    col = lax.broadcasted_iota(jnp.int32, (rows, heads), 1)
    return jnp.sum(jnp.where(row == col, wide, 0.0), axis=1, keepdims=True)


def group_read(spread, bias, keys, values):
    rows = spread.shape[0]
    chunks = keys.shape[0] // LANES
    score = lax.dot_general(
        spread, keys, (((1,), (1,)), ((), ())), preferred_element_type=jnp.float32
    )
    score = score + bias
    keep = -(jnp.maximum(score, 0.0) + jnp.log1p(jnp.exp(-jnp.abs(score))))
    stacked = jnp.concatenate(
        [keep[:, c * LANES:(c + 1) * LANES] for c in range(chunks)], axis=0
    )
    source = lax.broadcasted_iota(jnp.int32, (LANES, LANES), 0)
    target = lax.broadcasted_iota(jnp.int32, (LANES, LANES), 1)
    later = (source > target).astype(jnp.float32)
    inside = jnp.dot(stacked, later, precision=lax.Precision.HIGHEST)
    total = jnp.dot(stacked, jnp.ones_like(later), precision=lax.Precision.HIGHEST)
    carry = jnp.zeros((rows, LANES), jnp.float32)
    pieces = [None] * chunks
    for c in reversed(range(chunks)):
        pieces[c] = inside[c * rows:(c + 1) * rows] + carry
        carry = carry + total[c * rows:(c + 1) * rows]
    weight = jnp.exp(score + keep + jnp.concatenate(pieces, axis=1)).astype(jnp.bfloat16)
    read = jnp.dot(weight, values, preferred_element_type=jnp.float32)
    return read, jnp.broadcast_to(carry[:, 0:1], read.shape)


def exchange_kernel(
    n_sp, n_tp, repeat, x_hbm, gain_hbm, wk_hbm, wv_hbm, query_hbm, bias_hbm,
    land_ref, part_ref, x_buf, w_buf, gain_ref, query_ref, bias_ref, send_buf,
    x_sem, w_sem, small_sem, send_sem, recv_sem,
):
    sp, tp = lax.axis_index("sp"), lax.axis_index("tp")
    me = sp * n_tp + tp
    count = n_sp * n_tp
    span, cols = send_buf.shape[3], send_buf.shape[4]

    def sequence_at(i):
        return flip(sp, send_mask(n_sp, i), n_sp)

    def x_copy(i):
        return pltpu.make_async_copy(x_hbm.at[sequence_at(i)], x_buf.at[i], x_sem.at[i])

    def w_copy(which):
        source = (wk_hbm, wv_hbm)[which]
        return pltpu.make_async_copy(source, w_buf.at[which], w_sem.at[which])

    small = [
        pltpu.make_async_copy(source, buffer, small_sem.at[k])
        for k, (source, buffer) in enumerate(
            ((gain_hbm, gain_ref), (query_hbm, query_ref), (bias_hbm, bias_ref))
        )
    ]
    barrier = pltpu.get_barrier_semaphore()

    @pl.loop(1, count)
    def _(j):
        other = (me + j) % count
        pl.semaphore_signal(
            barrier, inc=1, device_id=(other // n_tp, other % n_tp), device_id_type=MESH
        )

    small[0].start()
    x_copy(0).start()
    w_copy(0).start()
    w_copy(1).start()
    small[1].start()
    small[2].start()

    @pl.loop(1, n_sp)
    def _(i):
        x_copy(i).start()

    for copy in small:
        copy.wait()
    gain = gain_ref[...].astype(jnp.float32).reshape(1, gain_ref.shape[0])

    def compute(i, first):
        x_copy(i).wait()
        wide = x_buf[i].astype(jnp.float32)
        scale = lax.rsqrt(jnp.mean(wide * wide, axis=-1, keepdims=True) + EPSILON)
        normed = (wide * scale * gain).astype(jnp.bfloat16)
        for which in range(2):
            if first:
                w_copy(which).wait()
            rows = jnp.dot(normed, w_buf[which], preferred_element_type=jnp.float32)
            rows = rows.astype(jnp.bfloat16)
            for g in range(n_tp):
                send_buf[i, g, which] = rows[:, g * cols:(g + 1) * cols]

    def own_rows(source):
        return pl.ds(pl.multiple_of(source * span, span), span)

    def send(i, g):
        return pltpu.make_async_remote_copy(
            src_ref=send_buf.at[i, g],
            dst_ref=land_ref.at[:, own_rows(me), :],
            send_sem=send_sem.at[i, g],
            recv_sem=recv_sem.at[sp, tp],
            device_id=(sequence_at(i), g),
            device_id_type=MESH,
        )

    def send_one(i, j):
        if j:
            send(i, flip(tp, j, n_tp)).start()
            return
        own = sequence_at(i) == sp

        @pl.when(jnp.logical_not(own))
        def _():
            send(i, tp).start()

        @pl.when(own)
        def _():
            land_ref[:, own_rows(me), :] = send_buf[i, tp]

    turns = list(range(1, n_tp)) + [0]
    now, later = turns[:n_tp // 2], turns[n_tp // 2:]

    compute(0, True)
    pl.semaphore_wait(barrier, count - 1)
    for j in now:
        send_one(0, j)

    @pl.loop(1, n_sp)
    def _(i):
        compute(i, False)
        for j, k in zip(now, later):
            send_one(i, j)
            send_one(i - 1, k)

    for k in later:
        send_one(n_sp - 1, k)

    heads = query_ref.shape[1] // HEAD_DIMENSION
    spread = spread_query(query_ref, heads, repeat, cols)
    bias = bias_column(bias_ref, spread.shape[0])
    group_rows = n_tp * span

    def arrive(source):
        for g in range(n_tp):
            @pl.when(source * n_tp + g != me)
            def _():
                pltpu.make_async_remote_copy(
                    src_ref=send_buf.at[0, 0],
                    dst_ref=land_ref.at[:, own_rows(source * n_tp + g), :],
                    send_sem=send_sem.at[0, 0],
                    recv_sem=recv_sem.at[source, g],
                    device_id=(source, g),
                    device_id_type=MESH,
                ).wait_recv()

    @pl.loop(0, n_sp - 1)
    def _(i):
        source = flip(sp, read_mask(n_sp, i), n_sp)
        arrive(source)
        at = pl.ds(pl.multiple_of(source * group_rows, group_rows), group_rows)
        read, total = group_read(spread, bias, land_ref[0, at, :], land_ref[1, at, :])
        part_ref[source, 0] = read
        part_ref[source, 1] = total

    part_ref[n_sp, 0] = spread.astype(jnp.float32)
    part_ref[n_sp, 1] = jnp.broadcast_to(bias, spread.shape)
    last = flip(sp, n_sp - 1, n_sp)
    part_ref[last] = jnp.zeros(part_ref.shape[1:], jnp.float32)

    @pl.loop(0, n_sp)
    def _(i):
        for j in range(1, n_tp):
            send(i, flip(tp, j, n_tp)).wait_send()

        @pl.when(sequence_at(i) != sp)
        def _():
            send(i, tp).wait_send()

    arrive(last)


def write_kernel(
    n_sp, repeat, land_ref, part_ref, key_out, value_out, read_ref, part, sem
):
    length, cols = land_ref.shape[1:]
    copies = []
    for which, out in enumerate((key_out, value_out)):
        for c in range(WRITES):
            at = pl.ds(c * (length // WRITES), length // WRITES)
            copies.append(
                pltpu.make_async_copy(land_ref.at[which, at], out.at[0, at], sem.at[which, c])
            )
    for copy in copies:
        copy.start()
    heads = read_ref.shape[1] // HEAD_DIMENSION
    group_rows = length // n_sp
    spread = part_ref[n_sp, 0].astype(jnp.bfloat16)
    bias = part_ref[n_sp, 1][:, 0:1]
    last = flip(lax.axis_index("sp"), n_sp - 1, n_sp)
    at = pl.ds(pl.multiple_of(last * group_rows, group_rows), group_rows)
    read, total = group_read(spread, bias, land_ref[0, at, :], land_ref[1, at, :])
    part[...] = part_ref[0:n_sp]
    part[last, 0] = read
    part[last, 1] = total
    after = jnp.zeros_like(total)
    whole = jnp.zeros_like(read)
    for p in reversed(range(n_sp)):
        whole = whole + jnp.exp(after) * part[p, 0]
        after = after + part[p, 1]
    pieces = []
    for h in range(heads):
        left = (h // repeat) * HEAD_DIMENSION
        pieces.append(whole[h:h + 1, left:left + HEAD_DIMENSION])
    read_ref[...] = jnp.concatenate(pieces, axis=1).astype(jnp.bfloat16)
    for copy in copies:
        copy.wait()


def body(n_sp, n_tp, inputs, norm_gain, key_weight, value_weight, query, head_bias):
    seqs, span, width = inputs.shape
    cols = key_weight.shape[1] // n_tp
    q_heads = query.shape[1] // HEAD_DIMENSION
    repeat = q_heads // (cols // HEAD_DIMENSION)
    length = span * n_sp * n_tp
    rows = q_heads + -q_heads % SUBLANES
    lanes = cols + -cols % LANES
    kept = 2 * length * lanes * 2 + (n_sp + 1) * 2 * rows * lanes * 4
    hbm = pl.BlockSpec(memory_space=pltpu.HBM)
    vmem = pl.BlockSpec(memory_space=pltpu.VMEM)
    landed, parts = pl.pallas_call(
        functools.partial(exchange_kernel, n_sp, n_tp, repeat),
        out_shape=(
            pltpu.VMEM((2, length, cols), jnp.bfloat16),
            pltpu.VMEM((n_sp + 1, 2, rows, cols), jnp.float32),
        ),
        in_specs=[hbm] * 6,
        out_specs=(vmem, vmem),
        scratch_shapes=[
            pltpu.VMEM((seqs, span, width), jnp.bfloat16),
            pltpu.VMEM((2, width, key_weight.shape[1]), jnp.bfloat16),
            pltpu.VMEM(norm_gain.shape, norm_gain.dtype),
            pltpu.VMEM(query.shape, query.dtype),
            pltpu.VMEM(head_bias.shape, head_bias.dtype),
            pltpu.VMEM((n_sp, n_tp, 2, span, cols), jnp.bfloat16),
            pltpu.SemaphoreType.DMA((n_sp,)),
            pltpu.SemaphoreType.DMA((2,)),
            pltpu.SemaphoreType.DMA((3,)),
            pltpu.SemaphoreType.DMA((n_sp, n_tp)),
            pltpu.SemaphoreType.DMA((n_sp, n_tp)),
        ],
        compiler_params=pltpu.CompilerParams(
            collective_id=0, has_side_effects=True, vmem_limit_bytes=VMEM_BYTES - kept
        ),
    )(inputs, norm_gain, key_weight, value_weight, query, head_bias)
    return pl.pallas_call(
        functools.partial(write_kernel, n_sp, repeat),
        out_shape=(
            jax.ShapeDtypeStruct((1, length, cols), jnp.bfloat16),
            jax.ShapeDtypeStruct((1, length, cols), jnp.bfloat16),
            jax.ShapeDtypeStruct((1, q_heads * HEAD_DIMENSION), jnp.bfloat16),
        ),
        in_specs=[vmem, vmem],
        out_specs=(hbm, hbm, vmem),
        scratch_shapes=[
            pltpu.VMEM((n_sp, 2, rows, cols), jnp.float32),
            pltpu.SemaphoreType.DMA((2, WRITES)),
        ],
        compiler_params=pltpu.CompilerParams(vmem_limit_bytes=16 * 2**20),
    )(landed, parts)


def solution(mesh):
    placed = (P(None, ("sp", "tp"), None), P(), P(), P(), P("sp", "tp"), P("tp"))
    return jax.shard_map(
        functools.partial(body, mesh.shape["sp"], mesh.shape["tp"]),
        mesh=mesh,
        in_specs=placed,
        out_specs=(P("sp", None, "tp"), P("sp", None, "tp"), P("sp", "tp")),
        check_vma=False,
    )
```
